512 devices in a mesh: sp: 128 (over z, x, core), tp: 4 (over y).
Axes of the slice: x: 4, y: 4, z: 16, core: 2. Of those that a mesh axis runs over, the one named last changes fastest.
Arguments:
- tokens: bfloat16 [32768, 2048], P(('sp', 'tp')), may hold values from -40 to 40
- w_query: bfloat16 [2048, 1024], P(None, 'tp'), may hold values from -0.125 to 0.125
- w_key: bfloat16 [2048, 256], P(None, 'tp'), may hold values from -0.125 to 0.125
- w_value: bfloat16 [2048, 256], P(None, 'tp'), may hold values from -0.125 to 0.125
- w_out: bfloat16 [1024, 2048], P('tp'), may hold values from -0.1875 to 0.1875
- cum_gate: float32 [16, 32768], P('tp', 'sp'), may hold values from -4684 to 0, as said below
Outputs:
- layer_out: bfloat16 [32768, 2048], P(('sp', 'tp'))
The draws below stay inside these ranges and needn't reach their ends.
Inputs may be any that keep to these rules, and one draw needn't show every extreme that they name: `cum_gate`: each head's row does not rise along the positions.
All inputs are finite; a program needn't handle non-finite values.
Results may differ from the reference program's by a relative error of at most 0.012.
Values may be sent and summed in bfloat16 or wider, within the bound.
No kernel may reach another device: no remote copies, remote signals or barrier semaphores. Data moves between devices by JAX's collectives and lax.ppermute only.
A program may use at most 64 MiB of HBM per device.

```python
import math
import jax
import jax.numpy as jnp
from jax import lax

D = 2048
H = 16
KVH = 4
HD = 64
TOK_DEV = 256
STREAM_LENGTH = 32768


def draw_tokens(key, part):
    keys = jax.random.split(key, 3)
    base = jnp.clip(jax.random.normal(keys[0], (STREAM_LENGTH, D), jnp.float32), -6.0, 6.0)
    direction = jnp.clip(jax.random.normal(keys[1], (D,), jnp.float32), -4.0, 4.0)
    level = jax.random.uniform(keys[2], (STREAM_LENGTH // TOK_DEV,), jnp.float32, -1.5, 1.5)
    shifted = jnp.repeat(level, TOK_DEV)
    result = base + shifted[:, None] * direction[None, :]
    return result.astype(jnp.bfloat16)


def draw_cum_gate(key, part):
    keys = jax.random.split(key, 6)
    order = jax.random.permutation(keys[0], H)
    gentle_fading_rate = order < H // 2
    whole_loss = jnp.exp(jax.random.uniform(keys[1], (H,), jnp.float32, math.log(0.3), math.log(1.0)))
    slow_rate = whole_loss / STREAM_LENGTH
    fast_rate = jnp.exp(jax.random.uniform(keys[2], (H,), jnp.float32, math.log(0.01), math.log(1.0 / 30.0)))
    rate = jnp.where(gentle_fading_rate, slow_rate, fast_rate)
    device_multiplier = jnp.exp(jax.random.uniform(keys[3], (STREAM_LENGTH // TOK_DEV,), jnp.float32, math.log(0.5), math.log(2.0)))
    factor_tokens = jnp.repeat(device_multiplier, TOK_DEV)
    rough = jax.random.uniform(keys[4], (H, STREAM_LENGTH), jnp.float32, 0.0, 2.0)
    log_forget_factor = -rate[:, None] * factor_tokens[None, :] * rough
    probe_indices = jax.random.randint(keys[5], (3,), 0, STREAM_LENGTH)
    objective_terms = jax.random.uniform(jax.random.fold_in(key, 9), (3,), jnp.float32, math.log(0.5), math.log(0.8))
    key_head_clusters = jnp.zeros((STREAM_LENGTH,), jnp.float32).at[probe_indices].add(objective_terms)
    log_forget_factor = log_forget_factor + jnp.where(gentle_fading_rate[:, None], key_head_clusters[None, :], 0.0)
    return jnp.cumsum(log_forget_factor, axis=1)


def level_of(rng, dims, cuts, low, largest):
    def one(position, blocks):
        heights = jax.random.uniform(jax.random.fold_in(jax.random.fold_in(rng, 6), position), (blocks,), jnp.float32, low / len(cuts), largest / len(cuts))
        return jnp.repeat(jnp.exp(heights), dims[position] // blocks).reshape((-1,) + (1,) * (len(dims) - position - 1))

    gain = one(*cuts[0])
    for cut in cuts[1:]:
        gain = gain * one(*cut)
    return gain


def scatter_about(key, extent, deviation, bound, cuts=(), kind=jnp.bfloat16):
    values = deviation * jax.random.normal(key, extent, jnp.float32)
    if cuts:
        values = values * level_of(key, extent, cuts, -0.22, 0.18)
    return jnp.clip(values, -bound, bound).astype(kind)


def setup_inputs(seed: int = 0) -> dict:
    key_of = jax.random.split(jax.random.key(seed), 7)
    tokens = draw_tokens(jax.random.fold_in(key_of[6], 71), 0)
    w_query = scatter_about(key_of[1], (D, H * HD), D ** -0.5, 0.125, ((1, 4),))
    w_key = scatter_about(key_of[2], (D, KVH * HD), D ** -0.5, 0.125, ((1, 4),))
    w_value = scatter_about(key_of[3], (D, KVH * HD), D ** -0.5, 0.125, ((1, 4),))
    w_out = scatter_about(key_of[4], (H * HD, D), (H * HD) ** -0.5, 0.1875, ((0, 4),))
    cum_gate = draw_cum_gate(jax.random.fold_in(key_of[6], 71), 0)
    return dict(tokens=tokens, w_query=w_query, w_key=w_key, w_value=w_value, w_out=w_out, cum_gate=cum_gate)


def reference(tokens, w_query, w_key, w_value, w_out, cum_gate):
    length_all = tokens.shape[0]
    queries = jnp.dot(tokens, w_query, preferred_element_type=jnp.float32).astype(jnp.bfloat16)
    key_proj = jnp.dot(tokens, w_key, preferred_element_type=jnp.float32).astype(jnp.bfloat16)
    values = jnp.dot(tokens, w_value, preferred_element_type=jnp.float32).astype(jnp.bfloat16)
    group_size = H // KVH
    block_rows = math.gcd(length_all, 256)
    block_count = length_all // block_rows
    score_factor = float(HD) ** -0.5
    keys_wide = key_proj.astype(jnp.float32).reshape(length_all, KVH, HD)
    values_wide = values.astype(jnp.float32).reshape(length_all, KVH, HD)
    cum_keys = cum_gate.reshape(KVH, group_size, length_all)
    query_blocks = queries.reshape(block_count, block_rows, KVH, group_size, HD)
    cum_blocks = cum_gate.reshape(KVH, group_size, block_count, block_rows).transpose(2, 0, 1, 3)
    starts = jnp.arange(block_count, dtype=jnp.int32) * block_rows
    key_pos = jnp.arange(length_all, dtype=jnp.int32)

    def attend(bundle):
        query_block, cum_block, offset = bundle
        scores = jnp.einsum('tkgd,skd->kgts', query_block.astype(jnp.float32), keys_wide) * score_factor
        scores = scores + (cum_block[..., None] - cum_keys[:, :, None, :])
        query_pos = offset + jnp.arange(block_rows, dtype=jnp.int32)
        scores = jnp.where(key_pos[None, :] <= query_pos[:, None], scores, -jnp.inf)
        row_max = jnp.max(scores, axis=-1, keepdims=True)
        weights = jnp.exp(scores - row_max)
        totals = jnp.sum(weights, axis=-1)
        rounded = lax.optimization_barrier(weights.astype(jnp.bfloat16)).astype(jnp.float32)
        attended = jnp.einsum('kgts,skd->kgtd', rounded, values_wide) / totals[..., None]
        return attended.astype(jnp.bfloat16).transpose(2, 0, 1, 3).reshape(block_rows, H * HD)

    attended = lax.map(attend, (query_blocks, cum_blocks, starts)).reshape(length_all, H * HD)
    return jnp.dot(attended, w_out, preferred_element_type=jnp.float32).astype(jnp.bfloat16)
```

```python
import functools

import jax
import jax.numpy as jnp
from jax import lax
from jax.experimental import pallas as pl
from jax.experimental.pallas import tpu as pltpu
from jax.sharding import Mesh, PartitionSpec as P

HD = 64
ROWS = 256
HALF = 128
GROUP = 4
KROWS = 80
VROWS = 72
NEG_START = -1e30
NEG_MASKED = -2e30
BF = jnp.bfloat16
F32 = jnp.float32
SWAP = ((0, 1), (1, 0))
VMEM = pl.BlockSpec(memory_space=pltpu.VMEM)
SMEM = pl.BlockSpec(memory_space=pltpu.SMEM)


def three_parts(x):
    high = x.astype(BF)
    rest = x - high.astype(F32)
    middle = rest.astype(BF)
    low = (rest - middle.astype(F32)).astype(BF)
    return high, middle, low


def project_kernel(x_ref, wq_ref, wk_ref, wv_ref, gate_ref, q_ref, kv_ref):
    x = x_ref[...]
    query = jnp.dot(x, wq_ref[...], preferred_element_type=F32)
    for part in range(2):
        rows = [query[y * 64 + part * 32 : y * 64 + part * 32 + 32] for y in range(4)]
        turned = jnp.concatenate(rows, axis=0).T.astype(BF)
        q_ref[part] = (turned.astype(F32) * 0.125).astype(BF)
    kv_ref[0:64] = jnp.dot(x, wk_ref[...], preferred_element_type=F32).T.astype(BF)
    kv_ref[KROWS : KROWS + 64] = jnp.dot(x, wv_ref[...], preferred_element_type=F32).T.astype(BF)
    high, middle, low = three_parts(-gate_ref[...])
    kv_ref[64:80] = jnp.concatenate([high, middle, low, jnp.zeros((4, ROWS), BF)], axis=0)


def project(x, w_query, w_key, w_value, gate):
    return pl.pallas_call(
        project_kernel,
        in_specs=[VMEM] * 5,
        out_specs=[VMEM] * 2,
        out_shape=[
            jax.ShapeDtypeStruct((2, GROUP * HD, HALF), BF),
            jax.ShapeDtypeStruct((KROWS + 64, ROWS), BF),
        ],
        cost_estimate=pl.CostEstimate(flops=2 * 256 * 2048 * 384, bytes_accessed=3 << 20, transcendentals=0),
        name="project",
    )(x, w_query, w_key, w_value, gate)


def attend_kernel(first, last, sc_ref, q_ref, kv_ref, *refs):
    if first:
        refs = list(refs)
    else:
        acc_in, top_in, *refs = refs
    if last:
        out_ref, acc, top, qa, ks, vs = refs
    else:
        acc, top, qa, ks, vs = refs
    if first:
        acc[...] = jnp.zeros_like(acc)
        top[...] = jnp.full(top.shape, NEG_START, F32)
    else:
        acc[...] = acc_in[...]
        top[...] = top_in[...]
    row = lax.broadcasted_iota(jnp.int32, (16, 512), 0)
    head = lax.broadcasted_iota(jnp.int32, (16, 512), 1) // HALF
    chooser = jnp.where((row < 12) & (row % 4 == head), 1.0, 0.0).astype(BF)
    for part in range(2):
        for xq in range(4):
            for h in range(GROUP):
                qa[part, xq, 0:64, h * HALF : (h + 1) * HALF] = q_ref[xq, part, h * HD : (h + 1) * HD, :]
            qa[part, xq, 64:80, :] = chooser
    for b in range(8):
        ks[b * ROWS : (b + 1) * ROWS, 0:KROWS] = kv_ref[b, 0:KROWS, :].astype(F32).T.astype(BF)
        vs[b, 0:64] = kv_ref[b, KROWS : KROWS + 64, :]
        vs[b, 64:72] = jnp.ones((8, ROWS), BF)

    def step(part, block, count, start):
        keys = ks[pl.ds(pl.multiple_of(block * ROWS, ROWS), count * ROWS), 0:KROWS]
        for xq in range(4):
            for side in range(2):
                cols = slice(side * 256, side * 256 + 256)
                scores = jnp.dot(keys, qa[part, xq, :, cols], preferred_element_type=F32)
                if start is not None:
                    key_pos = start + lax.broadcasted_iota(jnp.int32, scores.shape, 0)
                    lane = lax.broadcasted_iota(jnp.int32, (1, 256), 1) % HALF
                    query_pos = xq * 512 + sc_ref[5] + part * 32 + (lane // 32) * 64 + lane % 32
                    scores = jnp.where(key_pos <= query_pos, scores, NEG_MASKED)
                old = top[part, xq, :, cols]
                new = jnp.maximum(old, jnp.max(scores, axis=0, keepdims=True))
                weights = jnp.exp(scores - new).astype(BF)
                decay = jnp.exp(old - new)
                update = jnp.dot(vs[block], weights[0:ROWS], preferred_element_type=F32)
                for j in range(1, count):
                    update += jnp.dot(vs[block + j], weights[j * ROWS : (j + 1) * ROWS], preferred_element_type=F32)
                acc[part, xq, :, cols] = acc[part, xq, :, cols] * decay + update
                top[part, xq, :, cols] = new

    def one_part(part, carry):
        full = sc_ref[part]
        pairs = full // 2

        def pair(i, c):
            step(part, i * 2, 2, None)
            return c

        def single(i, c):
            step(part, i, 1, jnp.where(i < full, -1000000, sc_ref[4]))
            return c

        lax.fori_loop(0, pairs, pair, 0)
        lax.fori_loop(pairs * 2, full + sc_ref[2 + part], single, 0)
        return carry

    lax.fori_loop(0, 2, one_part, 0)
    if last:
        for part in range(2):
            for xq in range(4):
                total = acc[part, xq, 64:65, :]
                some = total > 0.0
                safe = jnp.where(some, total, 1.0)
                out_ref[xq, part, 0:64] = (acc[part, xq, 0:64, :] / safe).astype(BF)
                level = jnp.where(some, top[part, xq] + jnp.log(safe), NEG_START)
                high, middle, low = three_parts(level)
                out_ref[xq, part, 64:72] = jnp.concatenate([high, middle, low, jnp.zeros((5, 512), BF)], axis=0)


def attend(scalars, queries, kv, state, last):
    first = state is None
    args = [scalars, queries, kv] + ([] if first else list(state))
    acc_shape = (2, 4, VROWS, 512)
    top_shape = (2, 4, 1, 512)
    scratch = [
        pltpu.VMEM((2, 4, KROWS, 512), BF),
        pltpu.VMEM((8 * ROWS, 128), BF),
        pltpu.VMEM((8, VROWS, ROWS), BF),
    ]
    if last:
        out_shape = [jax.ShapeDtypeStruct((4, 2, VROWS, 512), BF)]
        scratch = [pltpu.VMEM(acc_shape, F32), pltpu.VMEM(top_shape, F32)] + scratch
    else:
        out_shape = [jax.ShapeDtypeStruct(acc_shape, F32), jax.ShapeDtypeStruct(top_shape, F32)]
    return pl.pallas_call(
        functools.partial(attend_kernel, first, last),
        in_specs=[SMEM] + [VMEM] * (len(args) - 1),
        out_specs=[VMEM] * len(out_shape),
        out_shape=out_shape,
        scratch_shapes=scratch,
        cost_estimate=pl.CostEstimate(flops=5_000_000_000, bytes_accessed=4 << 20, transcendentals=4 << 20),
        compiler_params=pltpu.CompilerParams(vmem_limit_bytes=40 << 20),
        name="attend",
    )(*args)


def combine_kernel(x_ref, o_ref):
    for part in range(2):
        levels = []
        for s in range(4):
            high, middle, low = (x_ref[s, part, 64 + j : 65 + j, :].astype(F32) for j in range(3))
            levels.append(high + middle + low)
        top = jnp.maximum(jnp.maximum(levels[0], levels[1]), jnp.maximum(levels[2], levels[3]))
        shares = [jnp.exp(level - top) for level in levels]
        total = shares[0] + shares[1] + shares[2] + shares[3]
        mixed = x_ref[0, part, 0:64, :].astype(F32) * shares[0]
        for s in range(1, 4):
            mixed += x_ref[s, part, 0:64, :].astype(F32) * shares[s]
        mixed = (mixed / total).astype(BF)
        for h in range(GROUP):
            o_ref[part, h * HD : (h + 1) * HD, :] = mixed[:, h * HALF : (h + 1) * HALF]


def combine(x):
    return pl.pallas_call(
        combine_kernel,
        in_specs=[VMEM],
        out_specs=VMEM,
        out_shape=jax.ShapeDtypeStruct((2, GROUP * HD, HALF), BF),
        cost_estimate=pl.CostEstimate(flops=1_000_000, bytes_accessed=1 << 20, transcendentals=0),
        name="combine",
    )(x)


def sent_to_all(x, axis):
    copies = jnp.broadcast_to(x, (lax.axis_size(axis), *x.shape))
    return lax.all_to_all(copies, axis, split_axis=0, concat_axis=0, tiled=True)


def per_device(tokens, w_query, w_key, w_value, w_out, cum_gate):
    zh, zl, x, c = (lax.axis_index(a) for a in ("zh", "zl", "x", "c"))
    plane = zh * 2 + zl
    mirror = [(i, 15 - i) for i in range(16)]
    rows = sent_to_all(tokens, "y").reshape(ROWS, -1)
    queries, kv = project(rows, w_query, w_key, w_value, cum_gate)
    moved = lax.ppermute(queries[1], ("zh", "zl"), mirror)
    same_own = lax.all_gather(kv, "zh", axis=0)
    other_own = lax.ppermute(same_own, "zl", SWAP)
    same_swapped = lax.ppermute(same_own, "c", SWAP)
    other_swapped = lax.ppermute(other_own, "c", SWAP)
    gathered = sent_to_all(jnp.stack([queries[0], moved]), "x").reshape(4, 2, GROUP * HD, HALF)
    state = None
    blocks = [(same_own, zl, c), (same_swapped, zl, 1 - c), (other_own, 1 - zl, c), (other_swapped, 1 - zl, 1 - c)]
    for number, (block, parity, side) in enumerate(blocks):
        scalars = jnp.stack(
            [
                (plane - parity + 1) // 2,
                (15 - plane - parity + 1) // 2,
                1 - (plane - parity) % 2,
                1 - (15 - plane - parity) % 2,
                x * 512 + side * ROWS,
                c * ROWS,
            ]
        ).astype(jnp.int32)
        state = attend(scalars, gathered, block, state, number == 3)
    shared = lax.all_to_all(state[0], "x", 0, 0, tiled=True)
    mixed = combine(shared)
    back = lax.ppermute(mixed[1], ("zh", "zl"), mirror)
    outs = []
    for half in (mixed[0], back):
        share = lax.dot_general(half, w_out, (((0,), (0,)), ((), ())), preferred_element_type=F32).astype(BF)
        pieces = lax.all_to_all(share.reshape(4, 32, -1), "y", 0, 0, tiled=True)
        outs.append(jnp.sum(pieces.astype(F32), axis=0).astype(BF))
    return jnp.concatenate(outs, axis=0)


def solution(mesh):
    fine = Mesh(mesh.devices.reshape(8, 2, 4, 2, 4), ("zh", "zl", "x", "c", "y"))
    sp = ("zh", "zl", "x", "c")
    placed = (
        P((*sp, "y"), None),
        P(None, "y"),
        P(None, "y"),
        P(None, "y"),
        P("y", None),
        P("y", sp),
    )
    return jax.shard_map(per_device, mesh=fine, in_specs=placed, out_specs=P((*sp, "y"), None), check_vma=False)
```

```python
import functools
import math

import jax
import jax.numpy as jnp
from jax import lax
from jax.experimental import pallas as pl
from jax.experimental.pallas import tpu as pltpu
from jax.sharding import Mesh, PartitionSpec as P

HD = 64
ROWS = 256
HALF = 128
GROUP = 4
KROWS = 80
QROWS = 144
VROWS = 72
LOG2E = math.log2(math.e)
JUMP_LIMIT = 64.0
NEG_START = -1e30
NEG_MASKED = -2e30
BF = jnp.bfloat16
F32 = jnp.float32
SWAP = ((0, 1), (1, 0))
VMEM = pl.BlockSpec(memory_space=pltpu.VMEM)
SMEM = pl.BlockSpec(memory_space=pltpu.SMEM)


def three_parts(x):
    high = x.astype(BF)
    rest = x - high.astype(F32)
    middle = rest.astype(BF)
    low = (rest - middle.astype(F32)).astype(BF)
    return high, middle, low


def packed(x):
    return jnp.concatenate([*three_parts(x), jnp.zeros(x.shape, BF)], axis=0)


def project_kernel(x_ref, wq_ref, wk_ref, wv_ref, gate_ref, q_ref, kv_ref):
    x = x_ref[...].reshape(ROWS, x_ref.shape[2])
    across = (((1,), (1,)), ((), ()))
    query = jnp.dot(x, wq_ref[...], preferred_element_type=F32)
    key = lax.dot_general(x, wk_ref[...], across, preferred_element_type=F32)
    levels = gate_ref[...] * -LOG2E
    for part in range(2):
        starts = [y * 64 + part * 32 for y in range(4)]
        turned = jnp.concatenate([query[at : at + 32] for at in starts], axis=0).T.astype(BF)
        q_ref[part, 0:256] = turned
        keys = jnp.concatenate([key[at : at + 32] for at in starts], axis=0).T.astype(BF).astype(F32)
        own = turned.astype(F32).reshape(GROUP, HD, HALF) * keys
        level = jnp.concatenate([levels[:, at : at + 32] for at in starts], axis=1)
        q_ref[part, 256:272] = packed(jnp.sum(own, axis=1) * (LOG2E * 0.125) + level)
    kv_ref[0:64] = lax.dot_general(wk_ref[...], x, across, preferred_element_type=F32).astype(BF)
    kv_ref[KROWS : KROWS + 64] = lax.dot_general(wv_ref[...], x, across, preferred_element_type=F32).astype(BF)
    kv_ref[64:80] = packed(levels)


def project(x, w_query, w_key, w_value, gate):
    return pl.pallas_call(
        project_kernel,
        in_specs=[VMEM] * 5,
        out_specs=[VMEM] * 2,
        out_shape=[
            jax.ShapeDtypeStruct((2, GROUP * HD + 16, HALF), BF),
            jax.ShapeDtypeStruct((KROWS + 64, ROWS), BF),
        ],
        cost_estimate=pl.CostEstimate(flops=2 * 256 * 2048 * 384, bytes_accessed=3 << 20, transcendentals=0),
        name="project",
    )(x, w_query, w_key, w_value, gate)


def attend_kernel(first, last, sc_ref, q0_ref, q1_ref, q2_ref, q3_ref, own_ref, swapped_ref, *refs):
    q_refs = (q0_ref, q1_ref, q2_ref, q3_ref)
    if first:
        refs = list(refs)
    else:
        acc_in, top_in, *refs = refs
    if last:
        out_ref, acc, top, *refs = refs
    else:
        acc, top, *refs = refs
    qa, ks, vs, saved_acc, saved_top, jump = refs
    if first:
        acc[...] = jnp.zeros_like(acc)
        for part in range(2):
            for xq in range(4):
                rows = q_refs[xq][part, 256:272, :].astype(F32)
                sums = rows[0:4] + rows[4:8] + rows[8:12]
                for h in range(GROUP):
                    top[part, xq, :, h * HALF : (h + 1) * HALF] = sums[h : h + 1]
    else:
        acc[...] = acc_in[...]
        top[...] = top_in[...]
    row = lax.broadcasted_iota(jnp.int32, (16, 512), 0)
    head = lax.broadcasted_iota(jnp.int32, (16, 512), 1) // HALF
    chooser = jnp.where((row < 12) & (row % 4 == head), 1.0, 0.0).astype(BF)
    for part in range(2):
        for xq in range(4):
            for h in range(GROUP):
                cols = slice(h * HALF, (h + 1) * HALF)
                scaled = q_refs[xq][part, h * HD : (h + 1) * HD, :].astype(F32) * (LOG2E * 0.125)
                high = scaled.astype(BF)
                qa[part, xq, 0:64, cols] = high
                qa[part, xq, 64:128, cols] = (scaled - high.astype(F32)).astype(BF)
            qa[part, xq, 128:144, :] = chooser
    for b in range(8):
        for side, ref in enumerate((own_ref, swapped_ref)):
            keys = ref[b, 0:KROWS, :].astype(F32)
            at = slice((2 * b + side) * ROWS, (2 * b + side + 1) * ROWS)
            ks[at, 0:QROWS] = jnp.concatenate([keys[0:64], keys], axis=0).T.astype(BF)
            cols = slice(side * ROWS, (side + 1) * ROWS)
            vs[b, 0:64, cols] = ref[b, KROWS : KROWS + 64, :]
            vs[b, 64:72, cols] = jnp.ones((8, ROWS), BF)

    def masked(scores, part, xq, start):
        key = lax.broadcasted_iota(jnp.int32, scores.shape, 0)
        key_pos = key + jnp.where(key < ROWS, start + sc_ref[5], start - sc_ref[5])
        lane = lax.broadcasted_iota(jnp.int32, (1, scores.shape[1]), 1) % HALF
        query_pos = sc_ref[6 + xq] * 512 + sc_ref[5] + part * 32 + (lane // 32) * 64 + lane % 32
        return jnp.where(key_pos <= query_pos, scores, NEG_MASKED)

    def careful_step(part, plane, start):
        keys = ks[pl.ds(pl.multiple_of(plane * 512, 512), 512), 0:QROWS]
        tiles = [(xq, slice(side * 256, side * 256 + 256)) for xq in range(4) for side in range(2)]

        def score(i):
            xq, cols = tiles[i]
            scores = jnp.dot(keys, qa[part, xq, :, cols], preferred_element_type=F32)
            return scores if start is None else masked(scores, part, xq, start)

        def soften(i, scores):
            xq, cols = tiles[i]
            old = top[part, xq, :, cols]
            new = jnp.maximum(old, jnp.max(scores, axis=0, keepdims=True))
            top[part, xq, :, cols] = new
            return jnp.exp2(scores - new).astype(BF), jnp.exp2(old - new)

        def gather(i, weights, decay):
            xq, cols = tiles[i]
            update = jnp.dot(vs[plane], weights, preferred_element_type=F32)
            acc[part, xq, :, cols] = acc[part, xq, :, cols] * decay + update

        waiting = score(0)
        pending = None
        for i in range(8):
            following = score(i + 1) if i < 7 else None
            if pending is not None:
                gather(i - 1, *pending)
            pending = soften(i, waiting)
            waiting = following
        gather(7, *pending)

    def quick_step(part, plane, start):
        keys = ks[pl.ds(pl.multiple_of(plane * 512, 512), 512), 0:QROWS]

        def soften(xq):
            scores = jnp.dot(keys, qa[part, xq], preferred_element_type=F32)
            if start is not None:
                scores = masked(scores, part, xq, start)
            old = top[part, xq]
            weights = jnp.exp2(scores - old).astype(BF)
            largest = jnp.max(scores, axis=0, keepdims=True)
            new = jnp.maximum(old, largest)
            top[part, xq] = new
            jump[...] = jnp.maximum(jump[...], largest - old)
            return weights, jnp.exp2(old - new)

        def gather(xq, weights, decay):
            update = jnp.dot(vs[plane], weights, preferred_element_type=F32)
            acc[part, xq] = (acc[part, xq] + update) * decay

        pending = soften(0)
        for xq in range(4):
            following = soften(xq + 1) if xq < 3 else None
            gather(xq, *pending)
            pending = following

    def one_part(part, carry):
        full = sc_ref[part]
        end = full + sc_ref[2 + part]

        def over(step):
            def whole(i, c):
                step(part, i, None)
                return c

            def edge(i, c):
                step(part, i, sc_ref[4])
                return c

            lax.fori_loop(0, full, whole, 0)
            lax.fori_loop(full, end, edge, 0)

        saved_acc[...] = acc[part]
        saved_top[...] = top[part]
        jump[...] = jnp.zeros_like(jump)
        over(quick_step)

        @pl.when(jnp.max(jump[...]) > JUMP_LIMIT)
        def _():
            acc[part] = saved_acc[...]
            top[part] = saved_top[...]
            over(careful_step)

        return carry

    lax.fori_loop(0, 2, one_part, 0)
    if last:
        for part in range(2):
            for xq in range(4):
                total = acc[part, xq, 64:65, :]
                some = total > 0.0
                safe = jnp.where(some, total, 1.0)
                out_ref[sc_ref[6 + xq], part, 0:64] = (acc[part, xq, 0:64, :] / safe).astype(BF)
                level = jnp.where(some, top[part, xq] + jnp.log2(safe), NEG_START)
                high, middle, low = three_parts(level)
                out_ref[sc_ref[6 + xq], part, 64:72] = jnp.concatenate([high, middle, low, jnp.zeros((5, 512), BF)], axis=0)


def attend(scalars, queries, own, swapped, state, last):
    first = state is None
    args = [scalars, *queries, own, swapped] + ([] if first else list(state))
    acc_shape = (2, 4, VROWS, 512)
    top_shape = (2, 4, 1, 512)
    scratch = [
        pltpu.VMEM((2, 4, QROWS, 512), BF),
        pltpu.VMEM((16 * ROWS, 256), BF),
        pltpu.VMEM((8, VROWS, 512), BF),
        pltpu.VMEM(acc_shape[1:], F32),
        pltpu.VMEM(top_shape[1:], F32),
        pltpu.VMEM((1, 512), F32),
    ]
    if last:
        out_shape = [jax.ShapeDtypeStruct((4, 2, VROWS, 512), BF)]
        scratch = [pltpu.VMEM(acc_shape, F32), pltpu.VMEM(top_shape, F32)] + scratch
    else:
        out_shape = [jax.ShapeDtypeStruct(acc_shape, F32), jax.ShapeDtypeStruct(top_shape, F32)]
    return pl.pallas_call(
        functools.partial(attend_kernel, first, last),
        in_specs=[SMEM] + [VMEM] * (len(args) - 1),
        out_specs=[VMEM] * len(out_shape),
        out_shape=out_shape,
        scratch_shapes=scratch,
        cost_estimate=pl.CostEstimate(flops=10_000_000_000, bytes_accessed=4 << 20, transcendentals=8 << 20),
        compiler_params=pltpu.CompilerParams(vmem_limit_bytes=40 << 20),
        name="attend",
    )(*args)


def combine_kernel(x_ref, o_ref):
    for part in range(2):
        levels = []
        for s in range(4):
            high, middle, low = (x_ref[s, part, 64 + j : 65 + j, :].astype(F32) for j in range(3))
            levels.append(high + middle + low)
        top = jnp.maximum(jnp.maximum(levels[0], levels[1]), jnp.maximum(levels[2], levels[3]))
        shares = [jnp.exp2(level - top) for level in levels]
        total = shares[0] + shares[1] + shares[2] + shares[3]
        mixed = x_ref[0, part, 0:64, :].astype(F32) * shares[0]
        for s in range(1, 4):
            mixed += x_ref[s, part, 0:64, :].astype(F32) * shares[s]
        mixed = (mixed / total).astype(BF)
        for h in range(GROUP):
            o_ref[part, h * HD : (h + 1) * HD, :] = mixed[:, h * HALF : (h + 1) * HALF]


def combine(x):
    return pl.pallas_call(
        combine_kernel,
        in_specs=[VMEM],
        out_specs=VMEM,
        out_shape=jax.ShapeDtypeStruct((2, GROUP * HD, HALF), BF),
        cost_estimate=pl.CostEstimate(flops=1_000_000, bytes_accessed=1 << 20, transcendentals=0),
        name="combine",
    )(x)


def sent_to_all(x, axis):
    copies = jnp.broadcast_to(x, (lax.axis_size(axis), *x.shape))
    return lax.all_to_all(copies, axis, split_axis=0, concat_axis=0, tiled=True)


def per_device(tokens, w_query, w_key, w_value, w_out, cum_gate):
    zh, zl, x, c = (lax.axis_index(a) for a in ("zh", "zl", "x", "c"))
    plane = zh * 2 + zl
    mirror = [(i, 15 - i) for i in range(16)]
    rows = sent_to_all(tokens, "y")
    queries, kv = project(rows, w_query, w_key.T, w_value.T, cum_gate)
    same_own = sent_to_all(kv, "zh")
    moved = lax.ppermute(queries[1], ("zh", "zl"), mirror)
    ours = jnp.stack([queries[0], moved])
    gathered = [ours] + [lax.ppermute(ours, "x", [(i, (i + j) % 4) for i in range(4)]) for j in (2, 1, 3)]
    gathered = [gathered[0], gathered[2], gathered[1], gathered[3]]
    same_own, gathered = lax.optimization_barrier((same_own, gathered))
    other_own = lax.ppermute(same_own, "zl", SWAP)
    same_swapped = lax.ppermute(same_own, "c", SWAP)
    state = None
    for number in range(2):
        parity = zl if number == 0 else 1 - zl
        scalars = jnp.stack(
            [
                (plane - parity + 1) // 2,
                (15 - plane - parity + 1) // 2,
                1 - (plane - parity) % 2,
                1 - (15 - plane - parity) % 2,
                x * 512,
                c * ROWS,
                *((x - j) % 4 for j in range(4)),
            ]
        ).astype(jnp.int32)
        if number == 0:
            state = attend(scalars, gathered, same_own, same_swapped, state, False)
        else:
            level, other_own = lax.optimization_barrier((state[1], other_own))
            state = (state[0], level)
            other_swapped = lax.ppermute(other_own, "c", SWAP)
            state = attend(scalars, gathered, other_own, other_swapped, state, True)
    shared = lax.all_to_all(state[0], "x", 0, 0, tiled=True)
    mixed = combine(shared)
    back = lax.ppermute(mixed[1], ("zh", "zl"), mirror)
    outs = []
    for half in (mixed[0], back):
        share = lax.dot_general(half, w_out, (((0,), (0,)), ((), ())), preferred_element_type=F32).astype(BF)
        pieces = lax.all_to_all(share.reshape(4, 32, -1), "y", 0, 0, tiled=True)
        outs.append(jnp.sum(pieces.astype(F32), axis=0).astype(BF))
    return jnp.concatenate(outs, axis=0)


def solution(mesh):
    fine = Mesh(mesh.devices.reshape(8, 2, 4, 2, 4), ("zh", "zl", "x", "c", "y"))
    sp = ("zh", "zl", "x", "c")
    placed = (
        P((*sp, "y"), None),
        P(None, "y"),
        P(None, "y"),
        P(None, "y"),
        P("y", None),
        P("y", sp),
    )
    return jax.shard_map(per_device, mesh=fine, in_specs=placed, out_specs=P((*sp, "y"), None), check_vma=False)
```

```python
import functools
import math

import jax
import jax.numpy as jnp
from jax import lax
from jax.experimental import pallas as pl
from jax.experimental.pallas import tpu as pltpu
from jax.sharding import Mesh, PartitionSpec as P

HD = 64
ROWS = 256
HALF = 128
GROUP = 4
KROWS = 80
QROWS = 144
VROWS = 72
LOG2E = math.log2(math.e)
JUMP_LIMIT = 64.0
NEG_START = -1e30
NEG_MASKED = -2e30
BF = jnp.bfloat16
F32 = jnp.float32
SWAP = ((0, 1), (1, 0))
VMEM = pl.BlockSpec(memory_space=pltpu.VMEM)
SMEM = pl.BlockSpec(memory_space=pltpu.SMEM)
HBM = pl.BlockSpec(memory_space=pltpu.HBM)


def three_parts(x):
    high = x.astype(BF)
    rest = x - high.astype(F32)
    middle = rest.astype(BF)
    low = (rest - middle.astype(F32)).astype(BF)
    return high, middle, low


def packed(x):
    return jnp.concatenate([*three_parts(x), jnp.zeros(x.shape, BF)], axis=0)


def project_kernel(x_ref, wq_ref, wk_ref, wv_ref, gate_ref, q_ref, kv_ref):
    x = x_ref[...].reshape(ROWS, x_ref.shape[2])
    across = (((1,), (1,)), ((), ()))
    query = jnp.dot(x, wq_ref[...], preferred_element_type=F32)
    key = lax.dot_general(x, wk_ref[...], across, preferred_element_type=F32)
    levels = gate_ref[...] * -LOG2E
    for part in range(2):
        starts = [y * 64 + part * 32 for y in range(4)]
        turned = jnp.concatenate([query[at : at + 32] for at in starts], axis=0).T.astype(BF)
        q_ref[part, 0:256] = turned
        keys = jnp.concatenate([key[at : at + 32] for at in starts], axis=0).T.astype(BF).astype(F32)
        own = turned.astype(F32).reshape(GROUP, HD, HALF) * keys
        level = jnp.concatenate([levels[:, at : at + 32] for at in starts], axis=1)
        q_ref[part, 256:272] = packed(jnp.sum(own, axis=1) * (LOG2E * 0.125) + level)
    keys = lax.dot_general(wk_ref[...], x, across, preferred_element_type=F32).astype(BF)
    values = lax.dot_general(wv_ref[...], x, across, preferred_element_type=F32).astype(BF)
    gates = packed(levels)
    for i in range(8):
        kv_ref[i, 0:64] = keys
        kv_ref[i, 64:80] = gates
        kv_ref[i, KROWS : KROWS + 64] = values


def project(x, w_query, w_key, w_value, gate):
    return pl.pallas_call(
        project_kernel,
        in_specs=[VMEM] * 5,
        out_specs=[VMEM] * 2,
        out_shape=[
            jax.ShapeDtypeStruct((2, GROUP * HD + 16, HALF), BF),
            jax.ShapeDtypeStruct((8, KROWS + 64, ROWS), BF),
        ],
        cost_estimate=pl.CostEstimate(flops=2 * 256 * 2048 * 384, bytes_accessed=3 << 20, transcendentals=0),
        name="project",
    )(x, w_query, w_key, w_value, gate)


def attend_kernel(parts, sc_ref, q0_ref, q1_ref, q2_ref, q3_ref, own_ref, swapped_ref, *refs):
    q_refs = (q0_ref, q1_ref, q2_ref, q3_ref)
    count = len(parts)
    first = count == 2
    if first:
        *outs, acc, top, qa, ks, vs, saved_acc, saved_top, jump, sems = refs
        acc[...] = jnp.zeros_like(acc)
        for part in parts:
            for xq in range(4):
                rows = q_refs[xq][part, 256:272, :].astype(F32)
                sums = rows[0:4] + rows[4:8] + rows[8:12]
                for h in range(GROUP):
                    top[part, xq, :, h * HALF : (h + 1) * HALF] = sums[h : h + 1]
    else:
        acc_in, top_in, out_ref, acc, top, qa, ks, vs, saved_acc, saved_top, jump, sems = refs
        fetch = pltpu.make_async_copy(acc_in, acc.at[0], sems.at[0])
        fetch.start()
        top[0] = top_in[...]
    row = lax.broadcasted_iota(jnp.int32, (16, 512), 0)
    head = lax.broadcasted_iota(jnp.int32, (16, 512), 1) // HALF
    chooser = jnp.where((row < 12) & (row % 4 == head), 1.0, 0.0).astype(BF)
    for slot, part in enumerate(parts):
        for xq in range(4):
            for h in range(GROUP):
                cols = slice(h * HALF, (h + 1) * HALF)
                scaled = q_refs[xq][part, h * HD : (h + 1) * HD, :].astype(F32) * (LOG2E * 0.125)
                high = scaled.astype(BF)
                qa[slot, xq, 0:64, cols] = high
                qa[slot, xq, 64:128, cols] = (scaled - high.astype(F32)).astype(BF)
            qa[slot, xq, 128:144, :] = chooser
    for b in range(8):
        for side, ref in enumerate((own_ref, swapped_ref)):
            keys = ref[b, 0:KROWS, :].astype(F32)
            at = slice((2 * b + side) * ROWS, (2 * b + side + 1) * ROWS)
            ks[at, 0:QROWS] = jnp.concatenate([keys[0:64], keys], axis=0).T.astype(BF)
            cols = slice(side * ROWS, (side + 1) * ROWS)
            vs[b, 0:64, cols] = ref[b, KROWS : KROWS + 64, :]
            vs[b, 64:72, cols] = jnp.ones((8, ROWS), BF)

    def masked(scores, part, xq, start):
        key = lax.broadcasted_iota(jnp.int32, scores.shape, 0)
        key_pos = key + jnp.where(key < ROWS, start + sc_ref[3], start - sc_ref[3])
        lane = lax.broadcasted_iota(jnp.int32, (1, scores.shape[1]), 1) % HALF
        query_pos = sc_ref[4 + xq] * 512 + sc_ref[3] + part * 32 + (lane // 32) * 64 + lane % 32
        return jnp.where(key_pos <= query_pos, scores, NEG_MASKED)

    def careful_step(slot, plane, start):
        keys = ks[pl.ds(pl.multiple_of(plane * 512, 512), 512), 0:QROWS]
        tiles = [(xq, slice(side * 256, side * 256 + 256)) for xq in range(4) for side in range(2)]

        def score(i):
            xq, cols = tiles[i]
            scores = jnp.dot(keys, qa[slot, xq, :, cols], preferred_element_type=F32)
            return scores if start is None else masked(scores, slot + parts[0], xq, start)

        def soften(i, scores):
            xq, cols = tiles[i]
            old = top[slot, xq, :, cols]
            new = jnp.maximum(old, jnp.max(scores, axis=0, keepdims=True))
            top[slot, xq, :, cols] = new
            return jnp.exp2(scores - new).astype(BF), jnp.exp2(old - new)

        def gather(i, weights, decay):
            xq, cols = tiles[i]
            update = jnp.dot(vs[plane], weights, preferred_element_type=F32)
            acc[slot, xq, :, cols] = acc[slot, xq, :, cols] * decay + update

        waiting = score(0)
        pending = None
        for i in range(8):
            following = score(i + 1) if i < 7 else None
            if pending is not None:
                gather(i - 1, *pending)
            pending = soften(i, waiting)
            waiting = following
        gather(7, *pending)

    def quick_step(slot, plane, start):
        keys = ks[pl.ds(pl.multiple_of(plane * 512, 512), 512), 0:QROWS]

        def soften(xq):
            scores = jnp.dot(keys, qa[slot, xq], preferred_element_type=F32)
            if start is not None:
                scores = masked(scores, slot + parts[0], xq, start)
            old = top[slot, xq]
            weights = jnp.exp2(scores - old).astype(BF)
            largest = jnp.max(scores, axis=0, keepdims=True)
            new = jnp.maximum(old, largest)
            top[slot, xq] = new
            jump[...] = jnp.maximum(jump[...], largest - old)
            return weights, jnp.exp2(old - new)

        def gather(xq, weights, decay):
            update = jnp.dot(vs[plane], weights, preferred_element_type=F32)
            acc[slot, xq] = (acc[slot, xq] + update) * decay

        pending = soften(0)
        for xq in range(4):
            following = soften(xq + 1) if xq < 3 else None
            gather(xq, *pending)
            pending = following

    def one_part(slot, carry):
        full = sc_ref[0]
        end = full + sc_ref[1]

        def over(step):
            def whole(i, c):
                step(slot, i, None)
                return c

            def edge(i, c):
                step(slot, i, sc_ref[2])
                return c

            lax.fori_loop(0, full, whole, 0)
            lax.fori_loop(full, end, edge, 0)

        saved_acc[...] = acc[slot]
        saved_top[...] = top[slot]
        jump[...] = jnp.zeros_like(jump)
        over(quick_step)

        @pl.when(jnp.max(jump[...]) > JUMP_LIMIT)
        def _():
            acc[slot] = saved_acc[...]
            top[slot] = saved_top[...]
            over(careful_step)

        return carry

    if not first:
        fetch.wait()
    lax.fori_loop(0, count, one_part, 0)
    if first:
        stores = [pltpu.make_async_copy(acc.at[part], outs[2 * part], sems.at[part]) for part in parts]
        for part in parts:
            stores[part].start()
            outs[2 * part + 1][...] = top[part]
        for part in parts:
            stores[part].wait()
    else:
        for xq in range(4):
            total = acc[0, xq, 64:65, :]
            some = total > 0.0
            safe = jnp.where(some, total, 1.0)
            out_ref[sc_ref[4 + xq], 0:64] = (acc[0, xq, 0:64, :] / safe).astype(BF)
            level = jnp.where(some, top[0, xq] + jnp.log2(safe), NEG_START)
            high, middle, low = three_parts(level)
            out_ref[sc_ref[4 + xq], 64:72] = jnp.concatenate([high, middle, low, jnp.zeros((5, 512), BF)], axis=0)


def attend(scalars, queries, own, swapped, parts, state):
    acc_shape = (4, VROWS, 512)
    top_shape = (4, 1, 512)
    if len(parts) == 2:
        out_shape = [jax.ShapeDtypeStruct(acc_shape, F32), jax.ShapeDtypeStruct(top_shape, F32)] * 2
    else:
        out_shape = [jax.ShapeDtypeStruct((4, VROWS, 512), BF)]
    args = [scalars, *queries, own, swapped, *state]
    return pl.pallas_call(
        functools.partial(attend_kernel, parts),
        in_specs=[SMEM] + [VMEM] * 6 + [HBM, VMEM][: len(state)],
        out_specs=[HBM, VMEM] * 2 if len(parts) == 2 else [VMEM],
        out_shape=out_shape,
        scratch_shapes=[
            pltpu.VMEM((len(parts), *acc_shape), F32),
            pltpu.VMEM((len(parts), *top_shape), F32),
            pltpu.VMEM((len(parts), 4, QROWS, 512), BF),
            pltpu.VMEM((16 * ROWS, 256), BF),
            pltpu.VMEM((8, VROWS, 512), BF),
            pltpu.VMEM(acc_shape, F32),
            pltpu.VMEM(top_shape, F32),
            pltpu.VMEM((1, 512), F32),
            pltpu.SemaphoreType.DMA((2,)),
        ],
        cost_estimate=pl.CostEstimate(flops=5_000_000_000 * len(parts), bytes_accessed=4 << 20, transcendentals=8 << 20),
        compiler_params=pltpu.CompilerParams(vmem_limit_bytes=24 << 20),
        name="attend",
    )(*args)


def merged(x_ref):
    levels = []
    for s in range(4):
        high, middle, low = (x_ref[s, 64 + j : 65 + j, :].astype(F32) for j in range(3))
        levels.append(high + middle + low)
    top = jnp.maximum(jnp.maximum(levels[0], levels[1]), jnp.maximum(levels[2], levels[3]))
    shares = [jnp.exp2(level - top) for level in levels]
    total = shares[0] + shares[1] + shares[2] + shares[3]
    mixed = x_ref[0, 0:64, :].astype(F32) * shares[0]
    for s in range(1, 4):
        mixed += x_ref[s, 0:64, :].astype(F32) * shares[s]
    return mixed / total


def finish_kernel(early_ref, late_ref, w_ref, o_ref):
    for part, ref in enumerate((early_ref, late_ref)):
        mixed = merged(ref)
        half = jnp.concatenate([mixed[:, h * HALF : (h + 1) * HALF] for h in range(GROUP)], axis=0)
        out = jnp.dot(half.T.astype(BF), w_ref[...], preferred_element_type=F32).astype(BF)
        for y in range(4):
            o_ref[y, part * 32 : part * 32 + 32, :] = out[y * 32 : y * 32 + 32]


def finish(early, late, w_out):
    return pl.pallas_call(
        finish_kernel,
        in_specs=[VMEM] * 3,
        out_specs=VMEM,
        out_shape=jax.ShapeDtypeStruct((4, 64, w_out.shape[1]), BF),
        cost_estimate=pl.CostEstimate(flops=300_000_000, bytes_accessed=3 << 20, transcendentals=0),
        name="finish",
    )(early, late, w_out)


def sent_to_all(x, axis):
    copies = jnp.broadcast_to(x, (lax.axis_size(axis), *x.shape))
    return lax.all_to_all(copies, axis, split_axis=0, concat_axis=0, tiled=True)


def per_device(tokens, w_query, w_key, w_value, w_out, cum_gate):
    zh, zl, x, c = (lax.axis_index(a) for a in ("zh", "zl", "x", "c"))
    plane = zh * 2 + zl
    rows = sent_to_all(tokens, "y")
    queries, copies = project(rows, w_query, w_key.T, w_value.T, cum_gate)
    same_own = lax.all_to_all(copies, "zh", 0, 0, tiled=True)
    two, one, three = (lax.ppermute(queries, "x", [(i, (i + j) % 4) for i in range(4)]) for j in (2, 1, 3))
    same_own, gathered = lax.optimization_barrier((same_own, [queries, one, two, three]))
    other_own = lax.ppermute(same_own, "zl", SWAP)
    same_swapped = lax.ppermute(same_own, "c", SWAP)
    scalars = []
    for parity in (zl, 1 - zl):
        full = (plane - parity + 1) // 2
        numbers = [full, 1 - (plane - parity) % 2, x * 512, c * ROWS, *((x - j) % 4 for j in range(4))]
        scalars.append(jnp.stack(numbers).astype(jnp.int32))
    acc0, top0, acc1, top1 = attend(scalars[0], gathered, same_own, same_swapped, (0, 1), ())
    top0, top1, other_own = lax.optimization_barrier((top0, top1, other_own))
    other_swapped = lax.ppermute(other_own, "c", SWAP)
    (late,) = attend(scalars[1], gathered, other_own, other_swapped, (1,), (acc1, top1))
    late_shared = lax.all_to_all(late, "x", 0, 0, tiled=True)
    (early,) = attend(scalars[1], gathered, other_own, other_swapped, (0,), (acc0, top0))
    early_shared = lax.all_to_all(early, "x", 0, 0, tiled=True)
    pieces = lax.all_to_all(finish(early_shared, late_shared, w_out), "y", 0, 0, tiled=True)
    return jnp.sum(pieces.astype(F32), axis=0).astype(BF)


def solution(mesh):
    fine = Mesh(mesh.devices.reshape(8, 2, 4, 2, 4), ("zh", "zl", "x", "c", "y"))
    sp = ("zh", "zl", "x", "c")
    placed = (
        P((*sp, "y"), None),
        P(None, "y"),
        P(None, "y"),
        P(None, "y"),
        P("y", None),
        P("y", sp),
    )
    return jax.shard_map(per_device, mesh=fine, in_specs=placed, out_specs=P((*sp, "y"), None), check_vma=False)
```

```python
import functools
import math

import jax
import jax.numpy as jnp
from jax import lax
from jax.experimental import pallas as pl
from jax.experimental.pallas import tpu as pltpu
from jax.sharding import Mesh, PartitionSpec as P

HD = 64
ROWS = 256
HALF = 128
GROUP = 4
KROWS = 80
QROWS = 144
VROWS = 72
LOG2E = math.log2(math.e)
JUMP_LIMIT = 64.0
ZERO_LIMIT = -160.0
NEG_START = -1e30
NEG_MASKED = -2e30
BF = jnp.bfloat16
F32 = jnp.float32
SWAP = ((0, 1), (1, 0))
VMEM = pl.BlockSpec(memory_space=pltpu.VMEM)
SMEM = pl.BlockSpec(memory_space=pltpu.SMEM)
HBM = pl.BlockSpec(memory_space=pltpu.HBM)


def three_parts(x):
    high = x.astype(BF)
    rest = x - high.astype(F32)
    middle = rest.astype(BF)
    low = (rest - middle.astype(F32)).astype(BF)
    return high, middle, low


def packed(x):
    return jnp.concatenate([*three_parts(x), jnp.zeros(x.shape, BF)], axis=0)


def project_kernel(x_ref, wq_ref, wk_ref, wv_ref, gate_ref, q_ref, kv_ref):
    x = x_ref[...].reshape(ROWS, x_ref.shape[2])
    across = (((1,), (1,)), ((), ()))
    query = jnp.dot(x, wq_ref[...], preferred_element_type=F32)
    both = lax.dot_general(jnp.concatenate([wk_ref[...], wv_ref[...]], axis=0), x, across, preferred_element_type=F32)
    keys = both[0:64].astype(BF)
    values = both[64:128].astype(BF)
    levels = gate_ref[...] * -LOG2E
    for part in range(2):
        starts = [y * 64 + part * 32 for y in range(4)]
        turned = jnp.concatenate([query[at : at + 32] for at in starts], axis=0).T.astype(BF)
        q_ref[part, 0:256] = turned
        own = jnp.concatenate([keys[:, at : at + 32].astype(F32) for at in starts], axis=1)
        own = turned.astype(F32).reshape(GROUP, HD, HALF) * own
        level = jnp.concatenate([levels[:, at : at + 32] for at in starts], axis=1)
        q_ref[part, 256:272] = packed(jnp.sum(own, axis=1) * (LOG2E * 0.125) + level)
    gates = packed(levels)
    for i in range(8):
        kv_ref[i, 0:64] = keys
        kv_ref[i, 64:80] = gates
        kv_ref[i, KROWS : KROWS + 64] = values


def project(x, w_query, w_key, w_value, gate):
    return pl.pallas_call(
        project_kernel,
        in_specs=[VMEM] * 5,
        out_specs=[VMEM] * 2,
        out_shape=[
            jax.ShapeDtypeStruct((2, GROUP * HD + 16, HALF), BF),
            jax.ShapeDtypeStruct((8, KROWS + 64, ROWS), BF),
        ],
        cost_estimate=pl.CostEstimate(flops=2 * 256 * 2048 * 384, bytes_accessed=3 << 20, transcendentals=0),
        name="project",
    )(x, w_query, w_key, w_value, gate)


def attend_kernel(parts, sc_ref, q0_ref, q1_ref, q2_ref, q3_ref, own_ref, swapped_ref, *refs):
    q_refs = (q0_ref, q1_ref, q2_ref, q3_ref)
    tiles = len(parts) * GROUP
    first = len(parts) == 2
    if first:
        *outs, acc, top, qa, ks, vs, jump, work, sems = refs
    else:
        acc_in, top_in, out_ref, acc, top, qa, ks, vs, jump, work, sems = refs

    def open_state():
        if first:
            acc[...] = jnp.zeros_like(acc)
            for slot, part in enumerate(parts):
                for xq in range(4):
                    rows = q_refs[xq][part, 256:272, :].astype(F32)
                    sums = rows[0:4] + rows[4:8] + rows[8:12]
                    for h in range(GROUP):
                        top[slot * GROUP + h, :, xq * HALF : (xq + 1) * HALF] = sums[h : h + 1]
        else:
            fetch = pltpu.make_async_copy(acc_in, acc.at[0:GROUP], sems.at[0])
            fetch.start()
            top[0:GROUP] = top_in[...]
            acc[GROUP] = jnp.zeros(acc.shape[1:], F32)
            fetch.wait()
        top[tiles] = jnp.zeros(top.shape[1:], F32)
        jump[...] = jnp.zeros_like(jump)

    open_state()
    row = lax.broadcasted_iota(jnp.int32, (16, 512), 0)
    query_sizes = []
    for slot, part in enumerate(parts):
        for h in range(GROUP):
            tile = slot * GROUP + h
            sizes = []
            for xq in range(4):
                cols = slice(xq * HALF, (xq + 1) * HALF)
                scaled = q_refs[xq][part, h * HD : (h + 1) * HD, :].astype(F32) * (LOG2E * 0.125)
                high = scaled.astype(BF)
                qa[tile, 0:64, cols] = high
                qa[tile, 64:128, cols] = (scaled - high.astype(F32)).astype(BF)
                sizes.append(jnp.sum(scaled * scaled, axis=0, keepdims=True))
            qa[tile, 128:144, :] = jnp.where((row < 12) & (row % 4 == h), 1.0, 0.0).astype(BF)
            query_sizes.append(jnp.max(jnp.concatenate(sizes, axis=1), axis=1, keepdims=True))
    qa[tiles] = jnp.zeros(qa.shape[1:], BF)
    key_sizes = []
    levels = []
    for b in range(8):
        sizes = []
        gates = []
        for side, ref in enumerate((own_ref, swapped_ref)):
            keys = ref[b, 0:KROWS, :].astype(F32)
            at = slice((2 * b + side) * ROWS, (2 * b + side + 1) * ROWS)
            ks[at, 0:QROWS] = jnp.concatenate([keys[0:64], keys], axis=0).T.astype(BF)
            cols = slice(side * ROWS, (side + 1) * ROWS)
            vs[b, 0:64, cols] = ref[b, KROWS : KROWS + 64, :]
            vs[b, 64:72, cols] = jnp.ones((8, ROWS), BF)
            sizes.append(jnp.sum(keys[0:64] * keys[0:64], axis=0, keepdims=True))
            gates.append(keys[64:68] + keys[68:72] + keys[72:76])
        key_sizes.append(jnp.maximum(sizes[0], sizes[1]))
        levels.append(jnp.maximum(gates[0], gates[1]))
    key_size = jnp.max(jnp.concatenate(key_sizes, axis=0), axis=1, keepdims=True)
    number = lax.broadcasted_iota(jnp.int32, (8, 1), 0)
    starts = []
    for tile in range(tiles):
        h = tile % GROUP
        level = jnp.max(jnp.concatenate([x[h : h + 1] for x in levels], axis=0), axis=1, keepdims=True)
        lowest = jnp.min(top[tile], axis=1, keepdims=True)
        bound = jnp.sqrt(key_size * query_sizes[tile]) * 1.01 + level - lowest
        starts.append(jnp.min(jnp.where(bound < ZERO_LIMIT, 8, number)))

    full = sc_ref[0]

    def enlist(plane, count):
        for tile in range(tiles):
            work[count] = plane * 16 + tile
            count = count + jnp.where(plane >= starts[tile], 1, 0)
        return count

    count = lax.fori_loop(0, full, enlist, 0)
    for j in range(3):
        work[count + j] = tiles

    def scored(plane, tile, start):
        keys = ks[pl.ds(pl.multiple_of(plane * 512, 512), 512), 0:QROWS]
        scores = jnp.dot(keys, qa[tile], preferred_element_type=F32)
        if start is None:
            return scores
        key = lax.broadcasted_iota(jnp.int32, scores.shape, 0)
        key_pos = key + jnp.where(key < ROWS, start + sc_ref[3], start - sc_ref[3])
        lane = lax.broadcasted_iota(jnp.int32, (1, 512), 1)
        base = jnp.where(
            lane < 256, jnp.where(lane < 128, sc_ref[4], sc_ref[5]), jnp.where(lane < 384, sc_ref[6], sc_ref[7])
        )
        inner = lane % HALF
        query_pos = base * 512 + sc_ref[3] + (parts[0] + tile // GROUP) * 32 + (inner // 32) * 64 + inner % 32
        return jnp.where(key_pos <= query_pos, scores, NEG_MASKED)

    def quick_step(pairs, start):
        def soften(i):
            plane, tile = pairs[i]
            scores = scored(plane, tile, start)
            old = top[tile]
            weights = jnp.exp2(scores - old).astype(BF)
            largest = jnp.max(scores, axis=0, keepdims=True)
            new = jnp.maximum(old, largest)
            top[tile] = new
            jump[...] = jnp.maximum(jump[...], largest - old)
            return weights, jnp.exp2(old - new)

        def gather(i, weights, decay):
            plane, tile = pairs[i]
            update = jnp.dot(vs[plane], weights, preferred_element_type=F32)
            acc[tile] = (acc[tile] + update) * decay

        pending = soften(0)
        for i in range(4):
            following = soften(i + 1) if i < 3 else None
            gather(i, *pending)
            pending = following

    def edge_unit(i, c):
        quick_step([(full, i * 4 + j) for j in range(4)], sc_ref[2])
        return c

    def work_unit(i, c):
        codes = [work[i * 4 + j] for j in range(4)]
        quick_step([(code // 16, code % 16) for code in codes], None)
        return c

    lax.fori_loop(0, sc_ref[1] * len(parts), edge_unit, 0)
    lax.fori_loop(0, (count + 3) // 4, work_unit, 0)

    @pl.when(jnp.max(jump[...]) > JUMP_LIMIT)
    def _():
        open_state()

        def careful(plane, start):
            def one_tile(tile, c):
                scores = scored(plane, tile, start)
                old = top[tile]
                new = jnp.maximum(old, jnp.max(scores, axis=0, keepdims=True))
                top[tile] = new
                update = jnp.dot(vs[plane], jnp.exp2(scores - new).astype(BF), preferred_element_type=F32)
                acc[tile] = acc[tile] * jnp.exp2(old - new) + update
                return c

            lax.fori_loop(0, tiles, one_tile, 0)

        def careful_whole(plane, c):
            careful(plane, None)
            return c

        def careful_edge(plane, c):
            careful(plane, sc_ref[2])
            return c

        lax.fori_loop(0, full, careful_whole, 0)
        lax.fori_loop(full, full + sc_ref[1], careful_edge, 0)

    if first:
        stores = [
            pltpu.make_async_copy(acc.at[part * GROUP : (part + 1) * GROUP], outs[2 * part], sems.at[part]) for part in parts
        ]
        for part in parts:
            stores[part].start()
            outs[2 * part + 1][...] = top[part * GROUP : (part + 1) * GROUP]
        for part in parts:
            stores[part].wait()
    else:
        for h in range(GROUP):
            total = acc[h, 64:65, :]
            some = total > 0.0
            safe = jnp.where(some, total, 1.0)
            rows = (acc[h, 0:64, :] / safe).astype(BF)
            high, middle, low = three_parts(jnp.where(some, top[h] + jnp.log2(safe), NEG_START))
            tail = jnp.concatenate([high, middle, low, jnp.zeros((5, 512), BF)], axis=0)
            for xq in range(4):
                cols = slice(xq * HALF, (xq + 1) * HALF)
                out_ref[sc_ref[4 + xq], 0:64, h * HALF : (h + 1) * HALF] = rows[:, cols]
                out_ref[sc_ref[4 + xq], 64:72, h * HALF : (h + 1) * HALF] = tail[:, cols]


def attend(scalars, queries, own, swapped, parts, state):
    tiles = len(parts) * GROUP
    acc_shape = (GROUP, VROWS, 512)
    top_shape = (GROUP, 1, 512)
    if len(parts) == 2:
        out_shape = [jax.ShapeDtypeStruct(acc_shape, F32), jax.ShapeDtypeStruct(top_shape, F32)] * 2
    else:
        out_shape = [jax.ShapeDtypeStruct((4, VROWS, 512), BF)]
    args = [scalars, *queries, own, swapped, *state]
    return pl.pallas_call(
        functools.partial(attend_kernel, parts),
        in_specs=[SMEM] + [VMEM] * 6 + [HBM, VMEM][: len(state)],
        out_specs=[HBM, VMEM] * 2 if len(parts) == 2 else [VMEM],
        out_shape=out_shape,
        scratch_shapes=[
            pltpu.VMEM((tiles + 1, *acc_shape[1:]), F32),
            pltpu.VMEM((tiles + 1, *top_shape[1:]), F32),
            pltpu.VMEM((tiles + 1, QROWS, 512), BF),
            pltpu.VMEM((16 * ROWS, 256), BF),
            pltpu.VMEM((8, VROWS, 512), BF),
            pltpu.VMEM((1, 512), F32),
            pltpu.SMEM((80,), jnp.int32),
            pltpu.SemaphoreType.DMA((2,)),
        ],
        cost_estimate=pl.CostEstimate(flops=5_000_000_000 * len(parts), bytes_accessed=4 << 20, transcendentals=8 << 20),
        compiler_params=pltpu.CompilerParams(vmem_limit_bytes=24 << 20),
        name="attend",
    )(*args)


def merged(x_ref):
    levels = []
    for s in range(4):
        high, middle, low = (x_ref[s, 64 + j : 65 + j, :].astype(F32) for j in range(3))
        levels.append(high + middle + low)
    top = jnp.maximum(jnp.maximum(levels[0], levels[1]), jnp.maximum(levels[2], levels[3]))
    shares = [jnp.exp2(level - top) for level in levels]
    total = shares[0] + shares[1] + shares[2] + shares[3]
    mixed = x_ref[0, 0:64, :].astype(F32) * shares[0]
    for s in range(1, 4):
        mixed += x_ref[s, 0:64, :].astype(F32) * shares[s]
    return mixed / total


def finish_kernel(early_ref, late_ref, w_ref, o_ref):
    for part, ref in enumerate((early_ref, late_ref)):
        mixed = merged(ref)
        half = jnp.concatenate([mixed[:, h * HALF : (h + 1) * HALF] for h in range(GROUP)], axis=0)
        out = jnp.dot(half.T.astype(BF), w_ref[...], preferred_element_type=F32).astype(BF)
        for y in range(4):
            o_ref[y, part * 32 : part * 32 + 32, :] = out[y * 32 : y * 32 + 32]


def finish(early, late, w_out):
    return pl.pallas_call(
        finish_kernel,
        in_specs=[VMEM] * 3,
        out_specs=VMEM,
        out_shape=jax.ShapeDtypeStruct((4, 64, w_out.shape[1]), BF),
        cost_estimate=pl.CostEstimate(flops=300_000_000, bytes_accessed=3 << 20, transcendentals=0),
        name="finish",
    )(early, late, w_out)


def sent_to_all(x, axis):
    copies = jnp.broadcast_to(x, (lax.axis_size(axis), *x.shape))
    return lax.all_to_all(copies, axis, split_axis=0, concat_axis=0, tiled=True)


def per_device(tokens, w_query, w_key, w_value, w_out, cum_gate):
    zh, zl, x, c = (lax.axis_index(a) for a in ("zh", "zl", "x", "c"))
    plane = zh * 2 + zl
    rows = sent_to_all(tokens, "y")
    queries, copies = project(rows, w_query, w_key.T, w_value.T, cum_gate)
    same_own = lax.all_to_all(copies, "zh", 0, 0, tiled=True)
    two, one, three = (lax.ppermute(queries, "x", [(i, (i + j) % 4) for i in range(4)]) for j in (2, 1, 3))
    same_own, gathered = lax.optimization_barrier((same_own, [queries, one, two, three]))
    other_own = lax.ppermute(same_own, "zl", SWAP)
    same_swapped = lax.ppermute(same_own, "c", SWAP)
    scalars = []
    for parity in (zl, 1 - zl):
        full = (plane - parity + 1) // 2
        numbers = [full, 1 - (plane - parity) % 2, x * 512, c * ROWS, *((x - j) % 4 for j in range(4))]
        scalars.append(jnp.stack(numbers).astype(jnp.int32))
    acc0, top0, acc1, top1 = attend(scalars[0], gathered, same_own, same_swapped, (0, 1), ())
    top0, top1, other_own = lax.optimization_barrier((top0, top1, other_own))
    other_swapped = lax.ppermute(other_own, "c", SWAP)
    (late,) = attend(scalars[1], gathered, other_own, other_swapped, (1,), (acc1, top1))
    late_shared = lax.all_to_all(late, "x", 0, 0, tiled=True)
    (early,) = attend(scalars[1], gathered, other_own, other_swapped, (0,), (acc0, top0))
    early_shared = lax.all_to_all(early, "x", 0, 0, tiled=True)
    pieces = lax.all_to_all(finish(early_shared, late_shared, w_out), "y", 0, 0, tiled=True)
    return jnp.sum(pieces.astype(F32), axis=0).astype(BF)


def solution(mesh):
    fine = Mesh(mesh.devices.reshape(8, 2, 4, 2, 4), ("zh", "zl", "x", "c", "y"))
    sp = ("zh", "zl", "x", "c")
    placed = (
        P((*sp, "y"), None),
        P(None, "y"),
        P(None, "y"),
        P(None, "y"),
        P("y", None),
        P("y", sp),
    )
    return jax.shard_map(per_device, mesh=fine, in_specs=placed, out_specs=P((*sp, "y"), None), check_vma=False)
```

```python
import functools
import math

import jax
import jax.numpy as jnp
from jax import lax
from jax.experimental import pallas as pl
from jax.experimental.pallas import tpu as pltpu
from jax.sharding import Mesh, PartitionSpec as P

HD = 64
ROWS = 256
HALF = 128
GROUP = 4
KROWS = 80
QROWS = 144
VROWS = 72
LOG2E = math.log2(math.e)
JUMP_LIMIT = 64.0
ZERO_LIMIT = -160.0
NEG_START = -1e30
NEG_MASKED = -2e30
BF = jnp.bfloat16
F32 = jnp.float32
SWAP = ((0, 1), (1, 0))
VMEM = pl.BlockSpec(memory_space=pltpu.VMEM)
SMEM = pl.BlockSpec(memory_space=pltpu.SMEM)
HBM = pl.BlockSpec(memory_space=pltpu.HBM)


def three_parts(x):
    high = x.astype(BF)
    rest = x - high.astype(F32)
    middle = rest.astype(BF)
    low = (rest - middle.astype(F32)).astype(BF)
    return high, middle, low


def packed(x):
    return jnp.concatenate([*three_parts(x), jnp.zeros(x.shape, BF)], axis=0)


def project_kernel(x_ref, wq_ref, wk_ref, wv_ref, gate_ref, q_ref, kv_ref):
    x = x_ref[...].reshape(ROWS, x_ref.shape[2])
    across = (((1,), (1,)), ((), ()))
    query = jnp.dot(x, wq_ref[...], preferred_element_type=F32)
    both = lax.dot_general(jnp.concatenate([wk_ref[...], wv_ref[...]], axis=0), x, across, preferred_element_type=F32)
    keys = both[0:64].astype(BF)
    values = both[64:128].astype(BF)
    levels = gate_ref[...] * -LOG2E
    for part in range(2):
        starts = [y * 64 + part * 32 for y in range(4)]
        turned = jnp.concatenate([query[at : at + 32] for at in starts], axis=0).T.astype(BF)
        q_ref[part, 0:256] = turned
        own = jnp.concatenate([keys[:, at : at + 32].astype(F32) for at in starts], axis=1)
        own = turned.astype(F32).reshape(GROUP, HD, HALF) * own
        level = jnp.concatenate([levels[:, at : at + 32] for at in starts], axis=1)
        q_ref[part, 256:272] = packed(jnp.sum(own, axis=1) * (LOG2E * 0.125) + level)
    gates = packed(levels)
    for i in range(8):
        kv_ref[i, 0:64] = keys
        kv_ref[i, 64:80] = gates
        kv_ref[i, KROWS : KROWS + 64] = values


def project(x, w_query, w_key, w_value, gate):
    return pl.pallas_call(
        project_kernel,
        in_specs=[VMEM] * 5,
        out_specs=[VMEM] * 2,
        out_shape=[
            jax.ShapeDtypeStruct((2, GROUP * HD + 16, HALF), BF),
            jax.ShapeDtypeStruct((8, KROWS + 64, ROWS), BF),
        ],
        cost_estimate=pl.CostEstimate(flops=2 * 256 * 2048 * 384, bytes_accessed=3 << 20, transcendentals=0),
        name="project",
    )(x, w_query, w_key, w_value, gate)


def attend_kernel(parts, sc_ref, q0_ref, q1_ref, q2_ref, q3_ref, own_ref, swapped_ref, *refs):
    q_refs = (q0_ref, q1_ref, q2_ref, q3_ref)
    tiles = len(parts) * GROUP
    first = len(parts) == 2
    if first:
        *outs, acc, top, qa, ks, vs, jump, work, sems = refs
    else:
        acc_in, top_in, out_ref, acc, top, qa, ks, vs, jump, work, sems = refs

    def open_state():
        if first:
            acc[...] = jnp.zeros_like(acc)
            for slot, part in enumerate(parts):
                for xq in range(4):
                    rows = q_refs[xq][part, 256:272, :].astype(F32)
                    sums = rows[0:4] + rows[4:8] + rows[8:12]
                    for h in range(GROUP):
                        top[slot * GROUP + h, :, xq * HALF : (xq + 1) * HALF] = sums[h : h + 1]
        else:
            fetch = pltpu.make_async_copy(acc_in, acc.at[0:GROUP], sems.at[0])
            fetch.start()
            top[0:GROUP] = top_in[...]
            acc[GROUP] = jnp.zeros(acc.shape[1:], F32)
            fetch.wait()
        top[tiles] = jnp.zeros(top.shape[1:], F32)
        jump[...] = jnp.zeros_like(jump)

    open_state()
    row = lax.broadcasted_iota(jnp.int32, (16, 512), 0)
    query_sizes = []
    for slot, part in enumerate(parts):
        for h in range(GROUP):
            tile = slot * GROUP + h
            sizes = []
            for xq in range(4):
                cols = slice(xq * HALF, (xq + 1) * HALF)
                scaled = q_refs[xq][part, h * HD : (h + 1) * HD, :].astype(F32) * (LOG2E * 0.125)
                high = scaled.astype(BF)
                qa[tile, 0:64, cols] = high
                qa[tile, 64:128, cols] = (scaled - high.astype(F32)).astype(BF)
                sizes.append(jnp.sum(scaled * scaled, axis=0, keepdims=True))
            qa[tile, 128:144, :] = jnp.where((row < 12) & (row % 4 == h), 1.0, 0.0).astype(BF)
            query_sizes.append(jnp.max(jnp.concatenate(sizes, axis=1), axis=1, keepdims=True))
    qa[tiles] = jnp.zeros(qa.shape[1:], BF)
    key_sizes = []
    levels = []
    for b in range(8):
        sizes = []
        gates = []
        for side, ref in enumerate((own_ref, swapped_ref)):
            keys = ref[b, 0:KROWS, :].astype(F32)
            at = slice((2 * b + side) * ROWS, (2 * b + side + 1) * ROWS)
            ks[at, 0:QROWS] = jnp.concatenate([keys[0:64], keys], axis=0).T.astype(BF)
            cols = slice(side * ROWS, (side + 1) * ROWS)
            vs[b, 0:64, cols] = ref[b, KROWS : KROWS + 64, :]
            vs[b, 64:72, cols] = jnp.ones((8, ROWS), BF)
            sizes.append(jnp.sum(keys[0:64] * keys[0:64], axis=0, keepdims=True))
            gates.append(keys[64:68] + keys[68:72] + keys[72:76])
        key_sizes.append(jnp.maximum(sizes[0], sizes[1]))
        levels.append(jnp.maximum(gates[0], gates[1]))
    key_size = jnp.max(jnp.concatenate(key_sizes, axis=0), axis=1, keepdims=True)
    number = lax.broadcasted_iota(jnp.int32, (8, 1), 0)
    starts = []
    for tile in range(tiles):
        h = tile % GROUP
        level = jnp.max(jnp.concatenate([x[h : h + 1] for x in levels], axis=0), axis=1, keepdims=True)
        lowest = jnp.min(top[tile], axis=1, keepdims=True)
        bound = jnp.sqrt(key_size * query_sizes[tile]) * 1.01 + level - lowest
        starts.append(jnp.min(jnp.where(bound < ZERO_LIMIT, 8, number)))

    full = sc_ref[0]

    def enlist(plane, count):
        for tile in range(tiles):
            work[count] = plane * 16 + tile
            count = count + jnp.where(plane >= starts[tile], 1, 0)
        return count

    count = lax.fori_loop(0, full, enlist, 0)
    for j in range(3):
        work[count + j] = tiles

    def scored(plane, tile, start):
        keys = ks[pl.ds(pl.multiple_of(plane * 512, 512), 512), 0:QROWS]
        scores = jnp.dot(keys, qa[tile], preferred_element_type=F32)
        if start is None:
            return scores
        key = lax.broadcasted_iota(jnp.int32, scores.shape, 0)
        key_pos = key + jnp.where(key < ROWS, start + sc_ref[3], start - sc_ref[3])
        lane = lax.broadcasted_iota(jnp.int32, (1, 512), 1)
        base = jnp.where(
            lane < 256, jnp.where(lane < 128, sc_ref[4], sc_ref[5]), jnp.where(lane < 384, sc_ref[6], sc_ref[7])
        )
        inner = lane % HALF
        query_pos = base * 512 + sc_ref[3] + (parts[0] + tile // GROUP) * 32 + (inner // 32) * 64 + inner % 32
        return jnp.where(key_pos <= query_pos, scores, NEG_MASKED)

    def quick_step(pairs, start):
        def soften(i):
            plane, tile = pairs[i]
            scores = scored(plane, tile, start)
            old = top[tile]
            weights = jnp.exp2(scores - old).astype(BF)
            largest = jnp.max(scores, axis=0, keepdims=True)
            new = jnp.maximum(old, largest)
            top[tile] = new
            jump[...] = jnp.maximum(jump[...], largest - old)
            return weights, jnp.exp2(old - new)

        def gather(i, weights, decay):
            plane, tile = pairs[i]
            update = jnp.dot(vs[plane], weights, preferred_element_type=F32)
            acc[tile] = (acc[tile] + update) * decay

        pending = soften(0)
        for i in range(4):
            following = soften(i + 1) if i < 3 else None
            gather(i, *pending)
            pending = following

    def edge_unit(i, c):
        quick_step([(full, i * 4 + j) for j in range(4)], sc_ref[2])
        return c

    def work_unit(i, c):
        codes = [work[i * 4 + j] for j in range(4)]
        quick_step([(code // 16, code % 16) for code in codes], None)
        return c

    lax.fori_loop(0, sc_ref[1] * len(parts), edge_unit, 0)
    lax.fori_loop(0, (count + 3) // 4, work_unit, 0)

    @pl.when(jnp.max(jump[...]) > JUMP_LIMIT)
    def _():
        open_state()

        def careful(plane, start):
            def one_tile(tile, c):
                scores = scored(plane, tile, start)
                old = top[tile]
                new = jnp.maximum(old, jnp.max(scores, axis=0, keepdims=True))
                top[tile] = new
                update = jnp.dot(vs[plane], jnp.exp2(scores - new).astype(BF), preferred_element_type=F32)
                acc[tile] = acc[tile] * jnp.exp2(old - new) + update
                return c

            lax.fori_loop(0, tiles, one_tile, 0)

        def careful_whole(plane, c):
            careful(plane, None)
            return c

        def careful_edge(plane, c):
            careful(plane, sc_ref[2])
            return c

        lax.fori_loop(0, full, careful_whole, 0)
        lax.fori_loop(full, full + sc_ref[1], careful_edge, 0)

    if first:
        stores = [
            pltpu.make_async_copy(acc.at[part * GROUP : (part + 1) * GROUP], outs[2 * part], sems.at[part]) for part in parts
        ]
        for part in parts:
            stores[part].start()
            outs[2 * part + 1][...] = top[part * GROUP : (part + 1) * GROUP]
        for part in parts:
            stores[part].wait()
    else:
        for h in range(GROUP):
            total = acc[h, 64:65, :]
            some = total > 0.0
            safe = jnp.where(some, total, 1.0)
            rows = (acc[h, 0:64, :] / safe).astype(BF)
            high, middle, low = three_parts(jnp.where(some, top[h] + jnp.log2(safe), NEG_START))
            tail = jnp.concatenate([high, middle, low, jnp.zeros((5, 512), BF)], axis=0)
            for xq in range(4):
                cols = slice(xq * HALF, (xq + 1) * HALF)
                out_ref[sc_ref[4 + xq], 0:64, h * HALF : (h + 1) * HALF] = rows[:, cols]
                out_ref[sc_ref[4 + xq], 64:72, h * HALF : (h + 1) * HALF] = tail[:, cols]


def attend(scalars, queries, own, swapped, parts, state):
    tiles = len(parts) * GROUP
    acc_shape = (GROUP, VROWS, 512)
    top_shape = (GROUP, 1, 512)
    if len(parts) == 2:
        out_shape = [jax.ShapeDtypeStruct(acc_shape, F32), jax.ShapeDtypeStruct(top_shape, F32)] * 2
    else:
        out_shape = [jax.ShapeDtypeStruct((4, VROWS, 512), BF)]
    args = [scalars, *queries, own, swapped, *state]
    return pl.pallas_call(
        functools.partial(attend_kernel, parts),
        in_specs=[SMEM] + [VMEM] * 6 + [HBM, VMEM][: len(state)],
        out_specs=[HBM, VMEM] * 2 if len(parts) == 2 else [VMEM],
        out_shape=out_shape,
        scratch_shapes=[
            pltpu.VMEM((tiles + 1, *acc_shape[1:]), F32),
            pltpu.VMEM((tiles + 1, *top_shape[1:]), F32),
            pltpu.VMEM((tiles + 1, QROWS, 512), BF),
            pltpu.VMEM((16 * ROWS, 256), BF),
            pltpu.VMEM((8, VROWS, 512), BF),
            pltpu.VMEM((1, 512), F32),
            pltpu.SMEM((80,), jnp.int32),
            pltpu.SemaphoreType.DMA((2,)),
        ],
        cost_estimate=pl.CostEstimate(flops=5_000_000_000 * len(parts), bytes_accessed=4 << 20, transcendentals=8 << 20),
        compiler_params=pltpu.CompilerParams(vmem_limit_bytes=24 << 20),
        name="attend",
    )(*args)


def merged(x_ref):
    levels = []
    for s in range(4):
        high, middle, low = (x_ref[s, 64 + j : 65 + j, :].astype(F32) for j in range(3))
        levels.append(high + middle + low)
    top = jnp.maximum(jnp.maximum(levels[0], levels[1]), jnp.maximum(levels[2], levels[3]))
    shares = [jnp.exp2(level - top) for level in levels]
    total = shares[0] + shares[1] + shares[2] + shares[3]
    mixed = x_ref[0, 0:64, :].astype(F32) * shares[0]
    for s in range(1, 4):
        mixed += x_ref[s, 0:64, :].astype(F32) * shares[s]
    return mixed / total


def regroup_kernel(early_ref, late_ref, o_ref):
    for part, ref in enumerate((early_ref, late_ref)):
        mixed = merged(ref)
        half = jnp.concatenate([mixed[:, h * HALF : (h + 1) * HALF] for h in range(GROUP)], axis=0)
        rows = half.T.astype(BF)
        for y in range(4):
            o_ref[y, part * 32 : part * 32 + 32, :] = rows[y * 32 : y * 32 + 32]


def regroup(early, late):
    return pl.pallas_call(
        regroup_kernel,
        in_specs=[VMEM] * 2,
        out_specs=VMEM,
        out_shape=jax.ShapeDtypeStruct((4, 64, GROUP * HD), BF),
        cost_estimate=pl.CostEstimate(flops=10_000_000, bytes_accessed=1 << 20, transcendentals=0),
        name="regroup",
    )(early, late)


def finish_kernel(sc_ref, x_ref, w0_ref, w1_ref, w2_ref, w3_ref, o_ref):
    total = None
    for j, ref in enumerate((w0_ref, w1_ref, w2_ref, w3_ref)):
        share = jnp.dot(x_ref[sc_ref[8 + j]], ref[...], preferred_element_type=F32)
        total = share if total is None else total + share
    o_ref[...] = total.astype(BF)


def finish(scalars, x, weights):
    return pl.pallas_call(
        finish_kernel,
        in_specs=[SMEM] + [VMEM] * 5,
        out_specs=VMEM,
        out_shape=jax.ShapeDtypeStruct((64, weights[0].shape[1]), BF),
        cost_estimate=pl.CostEstimate(flops=300_000_000, bytes_accessed=5 << 20, transcendentals=0),
        name="finish",
    )(scalars, x, *weights)


def sent_to_all(x, axis):
    copies = jnp.broadcast_to(x, (lax.axis_size(axis), *x.shape))
    return lax.all_to_all(copies, axis, split_axis=0, concat_axis=0, tiled=True)


def per_device(tokens, w_query, w_key, w_value, w_out, cum_gate):
    zh, zl, x, c = (lax.axis_index(a) for a in ("zh", "zl", "x", "c"))
    plane = zh * 2 + zl
    rows = sent_to_all(tokens, "y")
    queries, copies = project(rows, w_query, w_key.T, w_value.T, cum_gate)
    same_own = lax.all_to_all(copies, "zh", 0, 0, tiled=True)
    weights = [w_out]
    gathered = [queries]
    source, queries = lax.optimization_barrier((w_out, queries))
    for j in range(1, 4):
        shift = [(i, (i + j) % 4) for i in range(4)]
        weights.append(lax.ppermute(source, "y", shift))
        gathered.append(lax.ppermute(queries, "x", shift))
    same_own, gathered = lax.optimization_barrier((same_own, gathered))
    other_own = lax.ppermute(same_own, "zl", SWAP)
    same_swapped = lax.ppermute(same_own, "c", SWAP)
    scalars = []
    for parity in (zl, 1 - zl):
        full = (plane - parity + 1) // 2
        numbers = [full, 1 - (plane - parity) % 2, x * 512, c * ROWS]
        numbers += [(at - j) % 4 for at in (x, lax.axis_index("y")) for j in range(4)]
        scalars.append(jnp.stack(numbers).astype(jnp.int32))
    acc0, top0, acc1, top1 = attend(scalars[0], gathered, same_own, same_swapped, (0, 1), ())
    top0, top1, other_own = lax.optimization_barrier((top0, top1, other_own))
    other_swapped = lax.ppermute(other_own, "c", SWAP)
    (late,) = attend(scalars[1], gathered, other_own, other_swapped, (1,), (acc1, top1))
    late_shared = lax.all_to_all(late, "x", 0, 0, tiled=True)
    (early,) = attend(scalars[1], gathered, other_own, other_swapped, (0,), (acc0, top0))
    early_shared = lax.all_to_all(early, "x", 0, 0, tiled=True)
    pieces = lax.all_to_all(regroup(early_shared, late_shared), "y", 0, 0, tiled=True)
    return finish(scalars[1], pieces, weights)


def solution(mesh):
    fine = Mesh(mesh.devices.reshape(8, 2, 4, 2, 4), ("zh", "zl", "x", "c", "y"))
    sp = ("zh", "zl", "x", "c")
    placed = (
        P((*sp, "y"), None),
        P(None, "y"),
        P(None, "y"),
        P(None, "y"),
        P("y", None),
        P("y", sp),
    )
    return jax.shard_map(per_device, mesh=fine, in_specs=placed, out_specs=P((*sp, "y"), None), check_vma=False)
```
